128 devices in a mesh: sp: 32 (over z, y, core), tp: 4 (over x).
Axes of the slice: x: 4, y: 4, z: 4, core: 2. Of those that a mesh axis runs over, the one named last changes fastest.
Arguments:
- tokens: bfloat16 [2, 16384, 2048], P(None, ('sp', 'tp')), may hold values from -6.5 to 6.5, as said below
- norm_gain: float32 [2048], replicated, may hold values from 0.1 to 1.9
- w_gate: bfloat16 [2048, 4096], P('sp', 'tp'), may hold values from -0.125 to 0.125
- w_value: bfloat16 [2048, 4096], P('sp', 'tp'), may hold values from -0.125 to 0.125
- w_write: bfloat16 [2048, 512], P('sp', 'tp'), may hold values from -0.125 to 0.125
- w_read: bfloat16 [2048, 512], P('sp', 'tp'), may hold values from -0.125 to 0.125
- w_step: bfloat16 [2048, 64], replicated, may hold values from -0.125 to 0.125
- conv_value: float32 [4, 4096], replicated, may hold values from -3 to 3
- conv_write: float32 [4, 512], replicated, may hold values from -3 to 3
- conv_read: float32 [4, 512], replicated, may hold values from -3 to 3
- step_bias: float32 [64], replicated, as said below
- decay_log: float32 [64], replicated, may hold values from 0 to 0.7
- skip_gain: float32 [64], replicated, may hold values from 0.1 to 1.9
- out_gain: float32 [4096], replicated, may hold values from 0.1 to 1.9
- w_out: bfloat16 [4096, 2048], P(None, 'sp'), may hold values from -0.09375 to 0.09375
Outputs:
- mixed: bfloat16 [2, 16384, 2048], P(None, ('sp', 'tp'))
The draws below stay inside these ranges and needn't reach their ends.
Inputs may be any that keep to these rules, and one draw needn't show every extreme that they name: `tokens`: activations of order one whose mean along a direction drifts slowly over each sequence. `step_bias`: even heads take step offsets between -5.8 and -5.0, odd heads offsets near log(0.12 to 0.33) - log(16384).
All inputs are finite; a program needn't handle non-finite values.
Results may differ from the reference program's by a relative error of at most 0.005.
The reference program's roundings to bfloat16 on the way (of `normed`, `gated` and `mixed_in`) count: a program that leaves them out, or rounds other values in their place, can miss the bound.
Values may be sent and summed in bfloat16 or wider, within the bound.
No kernel may reach another device: no remote copies, remote signals or barrier semaphores. Data moves between devices by JAX's collectives and lax.ppermute only.
A program may use at most 192 MiB of HBM per device.

```python
import math
import jax
import jax.numpy as jnp
from jax import lax

D = 2048
HEADS = 64
HEAD_DIM = 64
GROUPS = 4
STATE = 128
CONV = 4
BLOCK = 64
SEQS = 2
HW = 4096
LENGTH = 16384


def draw_tokens(key, part):
    key_base, key_dir, key_phase, key_scale = jax.random.split(key, 4)
    base = jax.random.truncated_normal(key_base, -5.0, 5.0, (SEQS, LENGTH, D), jnp.float32)
    direction = jax.random.uniform(key_dir, (D,), jnp.float32, -1.0, 1.0)
    phase = jax.random.uniform(key_phase, (SEQS, 1), jnp.float32, 0.0, 6.283)
    position = jnp.arange(LENGTH, dtype=jnp.float32)[None, :] / LENGTH
    level = 1.5 * jnp.sin(18.85 * position + phase)
    return (base + level[..., None] * direction).astype(jnp.bfloat16)


def draw_step_bias(key, part):
    key_short, key_long = jax.random.split(key)
    short_mem = jax.random.uniform(key_short, (HEADS,), jnp.float32, -5.8, -5.0)
    long_mem = jax.random.uniform(key_long, (HEADS,), jnp.float32, math.log(0.12), math.log(0.33)) - math.log(LENGTH)
    parity = jnp.arange(HEADS) % 2
    return jnp.where(parity == 0, short_mem, long_mem)


def block_levels(stream_key, extent, cuts, low, top_value):
    level, own = 1.0, jax.random.fold_in(stream_key, 6)
    for axis_at, shards_of in cuts:
        heights = jnp.exp(jax.random.uniform(jax.random.fold_in(own, axis_at), (shards_of,), jnp.float32, low / len(cuts), top_value / len(cuts)))
        level = level * jnp.repeat(heights, extent[axis_at] // shards_of).reshape([-1 if axis == axis_at else 1 for axis in range(len(extent))])
    return level


def bell_draw(own_key, shape, deviation, limit, pieces=(), held_as=jnp.bfloat16):
    values = jax.random.normal(own_key, shape, jnp.float32) * deviation
    if len(pieces) > 0:
        values = block_levels(own_key, shape, pieces, -0.22, 0.18) * values
    return jnp.clip(values, min=-limit, max=limit).astype(held_as)


def setup_inputs(seed: int = 0) -> dict:
    key_of = jax.random.split(jax.random.key(seed), 16)
    tokens = draw_tokens(jax.random.fold_in(key_of[15], 71), 0)
    norm_gain = jnp.clip(1.0 + 0.18 * jax.random.normal(key_of[1], (D,), jnp.float32), 0.1, 1.9)
    w_gate = bell_draw(key_of[2], (D, HW), D ** -0.5, 0.125, ((0, 32), (1, 4)))
    w_value = bell_draw(key_of[3], (D, HW), D ** -0.5, 0.125, ((0, 32), (1, 4)))
    w_write = bell_draw(key_of[4], (D, GROUPS * STATE), D ** -0.5, 0.125, ((0, 32), (1, 4)))
    w_read = bell_draw(key_of[5], (D, GROUPS * STATE), D ** -0.5, 0.125, ((0, 32), (1, 4)))
    w_step = bell_draw(key_of[6], (D, HEADS), D ** -0.5, 0.125)
    conv_value = bell_draw(key_of[7], (CONV, HW), CONV ** -0.5, 3.0, (), jnp.float32)
    conv_write = bell_draw(key_of[8], (CONV, GROUPS * STATE), CONV ** -0.5, 3.0, (), jnp.float32)
    conv_read = bell_draw(key_of[9], (CONV, GROUPS * STATE), CONV ** -0.5, 3.0, (), jnp.float32)
    step_bias = draw_step_bias(jax.random.fold_in(key_of[15], 71), 0)
    decay_log = jnp.clip(jax.random.uniform(key_of[11], (HEADS,), jnp.float32, 0.0, 0.7), 0.0, 0.7)
    skip_gain = jnp.clip(1.0 + 0.18 * jax.random.normal(key_of[12], (HEADS,), jnp.float32), 0.1, 1.9)
    out_gain = jnp.clip(1.0 + 0.18 * jax.random.normal(key_of[13], (HW,), jnp.float32), 0.1, 1.9)
    w_out = bell_draw(key_of[14], (HW, D), HW ** -0.5, 0.09375, ((1, 32),))
    return {"tokens": tokens, "norm_gain": norm_gain, "w_gate": w_gate, "w_value": w_value, "w_write": w_write, "w_read": w_read, "w_step": w_step, "conv_value": conv_value, "conv_write": conv_write, "conv_read": conv_read, "step_bias": step_bias, "decay_log": decay_log, "skip_gain": skip_gain, "out_gain": out_gain, "w_out": w_out}


EPSILON = 1e-06
HIGHEST = lax.Precision.HIGHEST

def rms_scale(values, gain_vec):
    return values * lax.rsqrt(lax.optimization_barrier(jnp.mean(values * values, axis=-1, keepdims=True)) + EPSILON) * gain_vec

def causal_conv(values, kernel):
    tap_count = kernel.shape[0]
    length = values.shape[1]
    padded = jnp.pad(values, ((0, 0), (tap_count - 1, 0), (0, 0)))
    running = jnp.zeros_like(values)
    for offset in range(tap_count):
        running = running + padded[:, offset:offset + length, :] * kernel[offset]
    return jax.nn.silu(running)

def blockwise_state(value_conv, step_size, decay_rate, write_conv, read_conv):
    seq_count, length = (step_size.shape[0], step_size.shape[1])
    block_count = length // BLOCK
    repeat_heads = HEADS // GROUPS

    def split_blocks(values, tail_shape):
        return jnp.moveaxis(values.reshape((seq_count, block_count, BLOCK) + tail_shape), 1, 0)
    value_blocks = split_blocks(value_conv, (HEADS, HEAD_DIM))
    step_blocks = split_blocks(step_size, (HEADS,))
    write_blocks = split_blocks(write_conv, (GROUPS, STATE))
    read_blocks = split_blocks(read_conv, (GROUPS, STATE))
    causal_mask = jnp.arange(BLOCK)[:, None] >= jnp.arange(BLOCK)[None, :]

    def one_block(state, inputs):
        value_b, step_b, write_b, read_b = inputs
        write_heads = jnp.repeat(write_b, repeat_heads, axis=2)
        read_heads = jnp.repeat(read_b, repeat_heads, axis=2)
        log_decay = jnp.cumsum(step_b * decay_rate, axis=1)
        value_steps = value_b * step_b[..., None]
        log_gap = log_decay[:, :, None, :] - log_decay[:, None, :, :]
        weights = jnp.exp(jnp.where(causal_mask[None, :, :, None], log_gap, -jnp.inf))
        scores = jnp.einsum('slhn,smhn->slmh', read_heads, write_heads, precision=HIGHEST) * weights
        inner = jnp.einsum('slmh,smhp->slhp', scores, value_steps, precision=HIGHEST)
        carried = jnp.einsum('slhn,shpn->slhp', read_heads, state, precision=HIGHEST) * jnp.exp(log_decay)[..., None]
        block_decay = log_decay[:, -1, :]
        fade_out = jnp.exp(block_decay[:, None, :] - log_decay)
        state = state * jnp.exp(block_decay)[..., None, None] + jnp.einsum('smhn,smh,smhp->shpn', write_heads, fade_out, value_steps, precision=HIGHEST)
        return (state, inner + carried)
    initial = jnp.zeros((seq_count, HEADS, HEAD_DIM, STATE), jnp.float32)
    final_state, outputs = lax.scan(one_block, initial, (value_blocks, step_blocks, write_blocks, read_blocks))
    return jnp.moveaxis(outputs, 0, 1).reshape(seq_count, length, HEADS, HEAD_DIM)

def reference(tokens, norm_gain, w_gate, w_value, w_write, w_read, w_step, conv_value, conv_write, conv_read, step_bias, decay_log, skip_gain, out_gain, w_out):
    seq_count, length, model_width = tokens.shape
    flat_tokens = tokens.astype(jnp.float32).reshape(seq_count * length, model_width)
    normed = rms_scale(flat_tokens, norm_gain).astype(jnp.bfloat16)

    def project(weight):
        result = jnp.dot(normed, weight, preferred_element_type=jnp.float32).astype(jnp.bfloat16)
        result = lax.optimization_barrier(result)
        return result.reshape(seq_count, length, weight.shape[1])
    gate_in = project(w_gate)
    value_in = project(w_value)
    write_in = project(w_write)
    read_in = project(w_read)
    step_raw = jnp.dot(normed, w_step, preferred_element_type=jnp.float32).reshape(seq_count, length, HEADS)
    value_conv = causal_conv(value_in.astype(jnp.float32), conv_value)
    write_conv = causal_conv(write_in.astype(jnp.float32), conv_write)
    read_conv = causal_conv(read_in.astype(jnp.float32), conv_read)
    step_size = jax.nn.softplus(step_raw + step_bias)
    decay_rate = -jnp.exp(decay_log)
    heads_out = blockwise_state(value_conv, step_size, decay_rate, write_conv, read_conv)
    value_heads = value_conv.reshape(seq_count, length, HEADS, HEAD_DIM)
    heads_out = heads_out + skip_gain[:, None] * value_heads
    gated = (heads_out.reshape(seq_count, length, HW) * jax.nn.silu(gate_in.astype(jnp.float32))).astype(jnp.bfloat16)
    gated = lax.optimization_barrier(gated)
    mixed_in = rms_scale(gated.astype(jnp.float32), out_gain).astype(jnp.bfloat16)
    result = jnp.dot(mixed_in.reshape(seq_count * length, HW), w_out, preferred_element_type=jnp.float32)
    return result.astype(jnp.bfloat16).reshape(seq_count, length, model_width)
```

```python
import jax
import jax.numpy as jnp
from jax import lax
from jax.experimental import pallas as pl
from jax.experimental.pallas import tpu as pltpu
from jax.sharding import Mesh
from jax.sharding import PartitionSpec as P


SP = ("sp_0", "sp_1", "sp_2")
ALL = ("sp_0", "sp_1", "sp_2", "tp")
EPSILON = 1e-06
HIGHEST = lax.Precision.HIGHEST
BF = jnp.bfloat16
F32 = jnp.float32
CHUNK = 128
HALO = 16
NEG = -jnp.inf


def spot(z, y, c):
    return z * 8 + y * 2 + c


def sp_pairs(move):
    return [
        (spot(z, y, c), spot(*move(z, y, c)))
        for z in range(4)
        for y in range(4)
        for c in range(2)
    ]


def by_core(along_y, along_z, y_first):
    def move(z, y, c):
        if y_first == (c == 0):
            return (z, along_y(y), c)
        return (along_z(z), y, c)

    return move


def shift(by, y_first):
    along = lambda v: (v + by) % 4
    return by_core(along, along, y_first)


def flip(mask, y_first):
    along = lambda v: v ^ mask
    return by_core(along, along, y_first)


def other_core(z, y, c):
    return (z, y, 1 - c)


def sp_move(x, move):
    return lax.ppermute(x, SP, sp_pairs(move))


ORDERS = ((1, 3), (3, 1))


def gather_rows(shard, ahead=None, wait=None):
    got = [sp_move(shard, shift(by, True)) for by in (1, -1, 2)]
    if wait is not None:
        got, _ = lax.optimization_barrier((got, wait))
    held = [jnp.concatenate([shard, got[0]], axis=0), jnp.concatenate([got[1], got[2]], axis=0)]
    got = [sp_move(held[v], flip(ORDERS[v][0], False)) for v in range(2)]
    held = [jnp.concatenate([a, b], axis=0) for a, b in zip(held, got)]
    last = [sp_move(held[v], flip(ORDERS[v][1], False)) for v in range(2)]
    if ahead:
        (held, ahead) = lax.optimization_barrier((held, ahead()))
    near = [sp_move(held[v], other_core) for v in range(2)]
    far = [sp_move(last[v], other_core) for v in range(2)]
    return [held[0], last[0], held[1], last[1], near[0], far[0], near[1], far[1]], ahead


def slot_table():
    z, y, c = (lax.axis_index(a) for a in SP)
    chips = jnp.arange(16, dtype=jnp.int32)

    def place(first, second):
        d = second
        ends = ((d == 1) | (d == 2)).astype(jnp.int32)
        tops = (d >= 2).astype(jnp.int32)
        ring = jnp.where(first == 0, 0, jnp.where(first == 3, 1, jnp.where(first == 1, 2, 3)))
        one = jnp.where(ring < 2, ends, tops)
        two = jnp.where(ring < 2, tops, ends)
        return (ring // 2) * 8 + two * 4 + one * 2 + ring % 2

    y_first = place((chips % 4 - y) % 4, (chips // 4) ^ z)
    z_first = place((chips // 4 - z) % 4, (chips % 4) ^ y)
    own = jnp.where(c == 0, y_first, z_first)
    near = jnp.where(c == 0, z_first, y_first)
    table = jnp.stack([own, near], axis=1).reshape(32)
    return jnp.concatenate([table, jnp.stack([c, lax.axis_index("tp")]).astype(jnp.int32)])


def start_chip(table, chip, buffers, columns, into, sem):
    core = table[32]
    for k in range(2):
        slot = table[chip * 2 + k]
        whose = core if k == 0 else 1 - core
        target = into.at[pl.ds(pl.multiple_of(chip * 128 + whose * 64, 64), 64), :]
        here = pl.multiple_of((slot % 4) * 64, 64)
        for part in range(4):

            @pl.when(slot // 4 == part)
            def _(source=buffers[4 * k + part]):
                pltpu.make_async_copy(source.at[pl.ds(here, 64), columns], target, sem).start()


def wait_rows(into, at, rows, sem):
    part = into.at[pl.ds(at, rows), :]
    pltpu.make_async_copy(part, part, sem).wait()


def silu(v):
    return v / (1.0 + jnp.exp(-v))


def start_all(table, buffers, columns, into, sem):
    def one(chip, carry):
        start_chip(table, chip, buffers, columns, into, sem)
        return carry

    lax.fori_loop(0, 16, one, 0)


def norm_kernel(table, own, *rest):
    others, tails, gain, normed_ref = (rest[0:6:2], rest[1:6:2]), rest[6:10], rest[10], rest[11]
    tp = table[33]

    def norm_rows(load, seq, at, rows, step):
        def one(i, carry):
            part = load(pl.multiple_of(i * step, step)).astype(F32)
            scale = lax.rsqrt(jnp.mean(part * part, axis=-1, keepdims=True) + EPSILON)
            done = (part * scale * gain[...]).astype(BF)
            normed_ref[seq, pl.ds(pl.multiple_of(at + i * step, 16), step), :] = done
            return carry

        lax.fori_loop(0, rows // step, one, 0, unroll=rows // step < 3)

    for seq in range(2):
        for rank in range(4):

            @pl.when(tp == rank)
            def _():
                norm_rows(lambda r: tails[rank][seq], seq, 0, HALO, HALO)

        norm_rows(lambda r: own[seq, pl.ds(r, 32), :], seq, HALO + tp * 128, 128, 32)
        for ref, by in zip(others[seq], (3, 1, 2)):
            at = HALO + ((tp + by) % 4) * 128
            norm_rows(lambda r, ref=ref: ref[pl.ds(r, 32), :], seq, at, 128, 32)


def mix_kernel(table, normed_ref, *rest):
    weights, rest = rest[:8], rest[8:]
    (w_step, taps, bias, rate, skip, y_ref, read_ref, cum_ref, msg_ref) = rest[:9]
    w_one, w_two, proj, steps, cums, _, turned, fades, pairs, writes, state_ref, run, sems = rest[9:]
    seq, stage = pl.program_id(0), pl.program_id(1)

    @pl.when((seq == 0) & (stage == 0))
    def _():
        start_all(table, weights, pl.ds(0, 640), w_one, sems.at[0])
        start_all(table, weights, pl.ds(640, 640), w_two, sems.at[1])

    row = lax.broadcasted_iota(jnp.int32, (CHUNK, CHUNK), 0)
    col = lax.broadcasted_iota(jnp.int32, (CHUNK, CHUNK), 1)
    causal = row >= col
    left = col < 64

    def conv(r0, cols):
        at = r0 + HALO - 8
        rows = proj[pl.ds(at if isinstance(at, int) else pl.multiple_of(at, 8), CHUNK + 8), cols]
        acc = rows[5 : 5 + CHUNK] * taps[0:1, cols]
        for k in range(1, 4):
            acc = acc + rows[5 + k : 5 + k + CHUNK] * taps[k : k + 1, cols]
        return silu(acc)

    @pl.when(stage == 0)
    def _():
        for k, w_part in enumerate((w_one, w_two)):

            @pl.when(seq == 0)
            def _():
                wait_rows(w_part, 0, 2048, sems.at[k])

            cols = slice(k * 640, (k + 1) * 640)
            for r0, rows in ((0, HALO + 256), (HALO + 256, 256)):
                part = normed_ref[0, r0 : r0 + rows, :]
                proj[r0 : r0 + rows, cols] = (
                    jnp.dot(part, w_part[...], preferred_element_type=F32).astype(BF).astype(F32)
                )
                if k == 1:
                    steps[r0 : r0 + rows, :] = jnp.dot(
                        part, w_step[...], preferred_element_type=F32
                    )
        state_ref[...] = jnp.zeros((8, 128, 128), F32)
        run[...] = jnp.zeros((8, 128), F32)
        lower = jnp.where(causal, 1.0, 0.0).astype(F32)
        since = jnp.zeros((1, 128), F32)
        for c in range(4):
            rows = slice(c * CHUNK, (c + 1) * CHUNK)
            write = conv(c * CHUNK, pl.ds(1024, 128))
            read = conv(c * CHUNK, pl.ds(1152, 128))
            raw = steps[HALO + c * CHUNK : HALO + (c + 1) * CHUNK, :] + bias[...]
            step = jnp.maximum(raw, 0.0) + jnp.log1p(jnp.exp(-jnp.abs(raw)))
            cum = jnp.dot(lower, step * rate[...], precision=HIGHEST, preferred_element_type=F32)
            shifted = cum - jnp.log(step)
            cums[rows, :] = cum
            turned[rows, :] = shifted.T
            fades[rows, :] = jnp.exp(cum[CHUNK - 1 : CHUNK, :] - shifted)
            pairs[rows, :] = lax.dot_general(
                read, write, (((1,), (1,)), ((), ())), precision=HIGHEST, preferred_element_type=F32
            )
            writes[rows, :] = write.T.astype(BF)
            cum_ref[0, rows, :] = cum + since
            read_ref[0, rows, :] = read.astype(BF)
            since = since + cum[CHUNK - 1 : CHUNK, :]

    @pl.when(stage > 0)
    def _():
        r0 = pl.multiple_of((stage - 1) * CHUNK, CHUNK)
        rows = pl.ds(r0, CHUNK)
        cum = cums[rows, :]
        fade = fades[rows, :]
        shifted_t = turned[rows, :]
        pairing = pairs[rows, :]
        write_t = writes[rows, :]
        read_b = read_ref[0, rows, :]
        for p in range(8):
            cols = pl.ds(p * 128, 128)
            value = conv(r0, cols)
            value_b = value.astype(BF)
            zero = jnp.zeros_like(value_b)
            sides, tops, tails = [], [], []
            for h in (2 * p, 2 * p + 1):
                mine = jnp.broadcast_to(cum[:, h : h + 1], (CHUNK, CHUNK))
                gap = jnp.where(causal, mine - shifted_t[h : h + 1, :], NEG)
                sides.append((pairing * jnp.exp(gap)).astype(BF))
                tops.append(mine)
                tails.append(jnp.broadcast_to(fade[:, h : h + 1], (CHUNK, CHUNK)))
            both = jnp.concatenate(sides, axis=1)
            stacked = jnp.concatenate(
                [jnp.where(left, value_b, zero), jnp.where(left, zero, value_b)], axis=0
            )
            inner = jnp.dot(both, stacked, preferred_element_type=F32)
            decay = jnp.where(left, tops[0], tops[1])
            state = state_ref[p]
            carried = jnp.dot(read_b, state.astype(BF), preferred_element_type=F32)
            y_ref[0, :, cols] = inner + jnp.exp(decay) * carried + skip[:, cols] * value
            total = decay[CHUNK - 1 : CHUNK, :]
            scaled = (value * jnp.where(left, tails[0], tails[1])).astype(BF)
            state_ref[p] = state * jnp.exp(total) + jnp.dot(
                write_t, scaled, preferred_element_type=F32
            )
            run[p : p + 1, :] = run[p : p + 1, :] + total

    @pl.when(stage == 4)
    def _():
        line = lax.broadcasted_iota(jnp.int32, (16, 128), 0)
        for p in range(8):
            whole_decay = jnp.broadcast_to(run[p : p + 1, :], (16, 128))
            high = whole_decay.astype(BF).astype(F32)
            mid = (whole_decay - high).astype(BF).astype(F32)
            low = whole_decay - high - mid
            split = jnp.where(line == 0, high, jnp.where(line == 1, mid, jnp.where(line == 2, low, 0.0)))
            for k in range(2):
                msg_ref[2 * p + k, 0:64, :] = state_ref[p, k * 64 : (k + 1) * 64, :].astype(BF)
                msg_ref[2 * p + k, 64:80, :] = split.astype(BF)


def gate_kernel(table, normed, y_ref, cum_ref, *rest):
    weights = rest[:8]
    local_ref, scale_ref, w_gate, sem = rest[8:]

    @pl.when((pl.program_id(0) == 0) & (pl.program_id(1) == 0))
    def _():
        start_all(table, weights, pl.ds(1280, 1024), w_gate, sem)
        wait_rows(w_gate, 0, 2048, sem)

    at = pl.multiple_of(HALO + pl.program_id(1) * 256, 16)
    part = normed[0, pl.ds(at, 256), :]
    left = lax.broadcasted_iota(jnp.int32, (256, 128), 1) < 64
    decay = jnp.exp(cum_ref[0])
    for k in range(4):
        cols = slice(k * 256, (k + 1) * 256)
        raw = jnp.dot(part, w_gate[:, cols], preferred_element_type=F32).astype(BF).astype(F32)
        gate = silu(raw)
        local_ref[0, :, cols] = y_ref[0, :, cols] * gate
        for p in (2 * k, 2 * k + 1):
            spread = jnp.where(
                left,
                jnp.broadcast_to(decay[:, 2 * p : 2 * p + 1], (256, 128)),
                jnp.broadcast_to(decay[:, 2 * p + 1 : 2 * p + 2], (256, 128)),
            )
            half = slice((p % 2) * 128, (p % 2 + 1) * 128)
            scale_ref[0, :, p * 128 : (p + 1) * 128] = spread * gate[:, half]


def prefix_kernel(parts, out_ref):
    def one(i, held):
        out_ref[i] = held.astype(BF)
        decay = jnp.sum(parts[i, 64:80, :].astype(F32), axis=0, keepdims=True)
        return held * jnp.exp(decay) + parts[i, 0:64, :].astype(F32)

    lax.fori_loop(0, 32, one, jnp.zeros((64, 128), F32), unroll=4)


def join_kernel(local_ref, scale_ref, read_ref, state_ref, out_ref):
    for p in range(8):
        cols = slice(p * 128, (p + 1) * 128)
        carried = jnp.dot(read_ref[0], state_ref[0, p], preferred_element_type=F32)
        out_ref[0, 0, :, cols] = (
            local_ref[0, :, cols] + scale_ref[0, :, cols] * carried
        ).astype(BF)


def hold_kernel(table, *rest):
    weights, out_ref, sem = rest[:8], rest[8], rest[9]
    start_all(table, weights, slice(None), out_ref, sem)
    wait_rows(out_ref, 0, 2048, sem)


def out_kernel(parts, gain, w_out, out_ref, mixed):
    for seq in range(2):

        def norm(i, carry):
            rows = pl.ds(pl.multiple_of(i * 16, 16), 16)
            pieces = [parts[k, seq, rows, :].astype(F32) for k in range(4)]
            total = sum(jnp.sum(v * v, axis=-1, keepdims=True) for v in pieces)
            scale = lax.rsqrt(total * (1.0 / 4096) + EPSILON)
            into = pl.ds(pl.multiple_of(seq * 128 + i * 16, 16), 16)
            for k in range(4):
                cols = slice(k * 1024, (k + 1) * 1024)
                mixed[into, cols] = (pieces[k] * scale * gain[:, cols]).astype(BF)
            return carry

        lax.fori_loop(0, 8, norm, 0, unroll=2)
    for j in range(8):
        part = lax.dot_general(
            mixed[...],
            w_out[j * 256 : (j + 1) * 256, :],
            (((1,), (1,)), ((), ())),
            preferred_element_type=F32,
        ).astype(BF)
        out_ref[0, :, j * 256 : (j + 1) * 256] = part[:128]
        out_ref[1, :, j * 256 : (j + 1) * 256] = part[128:]


VMEM_SPEC = pl.BlockSpec(memory_space=pltpu.VMEM)
SMEM_SPEC = pl.BlockSpec(memory_space=pltpu.SMEM)
ANY_SPEC = pl.BlockSpec(memory_space=pl.ANY)


def whole(*shape):
    return pl.BlockSpec(shape, lambda *i: (0,) * len(shape))


def call(kernel, in_specs, outs, scratch=(), grid=(), out_specs=None, flops=0, room=58):
    return pl.pallas_call(
        kernel,
        grid=grid,
        in_specs=in_specs,
        out_specs=out_specs or [VMEM_SPEC] * len(outs),
        out_shape=[o if hasattr(o, "memory_space") else jax.ShapeDtypeStruct(*o) for o in outs],
        scratch_shapes=list(scratch),
        compiler_params=pltpu.CompilerParams(vmem_limit_bytes=room * 1024 * 1024),
        cost_estimate=pl.CostEstimate(flops=flops, bytes_accessed=1, transcendentals=0),
    )


def body(
    tokens,
    norm_gain,
    w_gate,
    w_value,
    w_write,
    w_read,
    w_step,
    conv_value,
    conv_write,
    conv_read,
    step_bias,
    decay_log,
    skip_gain,
    out_gain,
    w_out,
):
    tp = lax.axis_index("tp")

    def turn(x, by):
        return lax.ppermute(x, "tp", [(i, (i + by) % 4) for i in range(4)])

    prev_a = turn(tokens[0], 1)
    next_b = turn(tokens[1], -1)
    prev_b = turn(tokens[1], 1)
    next_a = turn(tokens[0], -1)
    far_a = turn(prev_a, 1)
    far_b = turn(next_b, -1)

    tails = []
    for k in range(4):
        pairs = [(g * 4 + 3, (g + 1) * 4 + k) for g in range(31)]
        tails.append(lax.ppermute(tokens[:, 128 - HALO :], ALL, pairs))

    def lanes(v):
        return jnp.pad(v, (0, 112)).reshape(1, 128)

    def heads_of(v):
        return lax.dynamic_slice_in_dim(v, tp * 16, 16, 0)

    def small():
        table = slot_table()
        step_cols = jnp.pad(lax.dynamic_slice_in_dim(w_step, tp * 16, 16, 1), ((0, 0), (0, 112)))
        taps = jnp.concatenate(
            [
                lax.dynamic_slice_in_dim(conv_value, tp * 1024, 1024, 1),
                lax.dynamic_slice_in_dim(conv_write, tp * 128, 128, 1),
                lax.dynamic_slice_in_dim(conv_read, tp * 128, 128, 1),
            ],
            axis=1,
        )
        bias = lanes(heads_of(step_bias))
        rate = lanes(-jnp.exp(heads_of(decay_log)))
        skip = jnp.repeat(heads_of(skip_gain), 64).reshape(1, 1024)
        return table, step_cols, taps, bias, rate, skip

    shard = jnp.concatenate([w_value, w_write, w_read, w_gate], axis=1)
    w_in, (table, step_cols, taps, bias, rate, skip) = gather_rows(shard, small)
    (normed,) = call(
        norm_kernel,
        [SMEM_SPEC] + [VMEM_SPEC] * 12,
        [((2, 512 + HALO, 2048), BF)],
        flops=5_000_000_000,
    )(
        table, tokens, prev_a, prev_b, next_a, next_b, far_a, far_b, *tails,
        norm_gain.reshape(1, 2048),
    )

    y_own, read, cum, pieces = call(
        mix_kernel,
        [SMEM_SPEC, pl.BlockSpec((1, 512 + HALO, 2048), lambda s, j: (s, 0, 0))]
        + [ANY_SPEC] * 8
        + [whole(2048, 128), whole(4, 1280), whole(1, 128), whole(1, 128), whole(1, 1024)],
        [
            ((2, 512, 1024), F32),
            ((2, 512, 128), BF),
            ((2, 512, 128), F32),
            ((32, 80, 128), BF),
        ],
        [
            pltpu.VMEM((2048, 640), BF),
            pltpu.VMEM((2048, 640), BF),
            pltpu.VMEM((512 + HALO, 1280), F32),
            pltpu.VMEM((512 + HALO, 128), F32),
            pltpu.VMEM((512, 128), F32),
            pltpu.VMEM((512, 128), F32),
            pltpu.VMEM((512, 128), F32),
            pltpu.VMEM((512, 128), F32),
            pltpu.VMEM((512, 128), F32),
            pltpu.VMEM((512, 128), BF),
            pltpu.VMEM((8, 128, 128), F32),
            pltpu.VMEM((8, 128), F32),
            pltpu.SemaphoreType.DMA((2,)),
        ],
        (2, 5),
        [
            pl.BlockSpec((1, CHUNK, 1024), lambda s, j: (s, jnp.maximum(j - 1, 0), 0)),
            pl.BlockSpec((1, 512, 128), lambda s, j: (s, 0, 0)),
            pl.BlockSpec((1, 512, 128), lambda s, j: (s, 0, 0)),
            pl.BlockSpec((16, 80, 128), lambda s, j: (s, 0, 0)),
        ],
        20_000_000_000,
    )(
        table, normed, *w_in, step_cols, taps, bias, rate, skip,
    )

    def quarter(width):
        return pl.BlockSpec((1, 256, width), lambda s, r: (s, r, 0))

    local, scale = call(
        gate_kernel,
        [SMEM_SPEC, pl.BlockSpec((1, 512 + HALO, 2048), lambda s, r: (s, 0, 0))]
        + [quarter(1024), quarter(128)]
        + [ANY_SPEC] * 8,
        [((2, 512, 1024), F32), ((2, 512, 1024), F32)],
        [pltpu.VMEM((2048, 1024), BF), pltpu.SemaphoreType.DMA(())],
        (2, 2),
        [quarter(1024), quarter(1024)],
        8_000_000_000,
    )(table, normed, y_own, cum, *w_in)

    w_back, _ = gather_rows(w_out.T, wait=read)

    pieces = lax.all_to_all(pieces, SP, split_axis=0, concat_axis=0, tiled=True)
    (before,) = call(prefix_kernel, [VMEM_SPEC], [((32, 64, 128), BF)])(pieces)
    entering = lax.all_to_all(before, SP, split_axis=0, concat_axis=0, tiled=True)

    def rows_of(width):
        return pl.BlockSpec((1, CHUNK, width), lambda s, r: (s, r, 0))

    (gated,) = call(
        join_kernel,
        [
            rows_of(1024),
            rows_of(1024),
            rows_of(128),
            pl.BlockSpec((1, 8, 128, 128), lambda s, r: (s, 0, 0, 0)),
        ],
        [((4, 2, 128, 1024), BF)],
        (),
        (2, 4),
        [pl.BlockSpec((1, 1, CHUNK, 1024), lambda s, r: (r, s, 0, 0))],
        4_000_000_000,
    )(local, scale, read, entering.reshape(2, 8, 128, 128))
    parts = lax.all_to_all(gated, "tp", split_axis=0, concat_axis=0, tiled=True)

    (w_held,) = call(
        hold_kernel,
        [SMEM_SPEC] + [ANY_SPEC] * 8,
        [pltpu.VMEM((2048, 4096), BF)],
        [pltpu.SemaphoreType.DMA(())],
        flops=4_000_000_000,
        room=8,
    )(table, *w_back)
    (mixed,) = call(
        out_kernel,
        [VMEM_SPEC] * 3,
        [((2, 128, 2048), BF)],
        [pltpu.VMEM((256, 4096), BF)],
        flops=8_000_000_000,
        room=32,
    )(parts, out_gain.reshape(1, 4096), w_held)
    return mixed


def solution(mesh):
    split = Mesh(mesh.devices.reshape(4, 4, 2, mesh.shape["tp"]), ("sp_0", "sp_1", "sp_2", "tp"))
    placed = (
        P(None, ALL, None),
        P(),
        P(SP, "tp"),
        P(SP, "tp"),
        P(SP, "tp"),
        P(SP, "tp"),
        P(),
        P(),
        P(),
        P(),
        P(),
        P(),
        P(),
        P(),
        P(None, SP),
    )
    return jax.shard_map(
        body, mesh=split, in_specs=placed, out_specs=P(None, ALL, None), check_vma=False
    )
```
